32 devices in a mesh: sp: 8 (over z, y), tp: 4 (over x, core).
Axes of the slice: x: 2, y: 2, z: 4, core: 2. Of those that a mesh axis runs over, the one named last changes fastest.
Arguments:
- queries: bfloat16 [5120, 1024], P('sp', 'tp'), may hold values from -6 to 6
- key_input: bfloat16 [5120, 1024], P('sp', 'tp'), may hold values from -6 to 6
- value_input: bfloat16 [5120, 1024], P('sp', 'tp'), may hold values from -6 to 6
- gate_input: bfloat16 [5120, 1024], P('sp', 'tp'), may hold values from -6 to 6
- log_decay: float32 [8, 5120], P('tp', 'sp'), may hold values from -1.6703125 to 0, as said below
- residual: bfloat16 [5120, 2048], P('sp'), may hold values from -52 to 52
- out_weight: bfloat16 [1024, 2048], P('tp'), may hold values from -0.375 to 0.375
- norm_gain: float32 [2048], replicated, may hold values from 0.3 to 2.7, as said below
- norm_bias: float32 [2048], replicated, may hold values from -1.8 to 1.8
- gate_weight: bfloat16 [2048, 5632], P('sp', 'tp'), may hold values from -0.125 to 0.125
- up_weight: bfloat16 [2048, 5632], P('sp', 'tp'), may hold values from -0.125 to 0.125
- down_weight: bfloat16 [5632, 2048], P('tp', 'sp'), may hold values from -0.078125 to 0.078125
- final_gain: float32 [2048], replicated, may hold values from 0.1 to 1.9
- final_bias: float32 [2048], replicated, may hold values from -1.8 to 1.8
Outputs:
- updated: bfloat16 [5120, 2048], P('sp', 'tp')
The draws below stay inside these ranges and needn't reach their ends.
Inputs may be any that keep to these rules, and one draw needn't show every extreme that they name: `log_decay`: log-decays, never positive. `norm_gain`: positive gains.
All inputs are finite; a program needn't handle non-finite values.
Results may differ from the reference program's by a relative error of at most 0.023.
Values may be sent and summed in bfloat16 or wider, within the bound.
A program may use at most 128 MiB of HBM per device.

```python
import jax
import jax.numpy as jnp
from jax import lax

D = 2048
HEADS = 8
HD = 128
FF = 5632
BLOCK = 128
TOK_DEV = 640
SEQ = 5120
N_SP = 8
N_TP = 4


def draw_log_decay(key, part):
    keys = jax.random.split(jax.random.fold_in(key, 7), 6)
    order = jax.random.permutation(keys[0], HEADS)
    fast_count = HEADS // 2
    fast = (order < fast_count)[:, None]
    fast_rate = jnp.exp(jax.random.uniform(keys[1], (HEADS, 1), jnp.float32, jnp.log(1.3), jnp.log(4.3))) / BLOCK
    gentle_attenuation = jnp.exp(jax.random.uniform(keys[2], (HEADS, 1), jnp.float32, jnp.log(0.1), jnp.log(0.5))) / SEQ
    fading_pace = jnp.where(fast, fast_rate, gentle_attenuation)
    fading_coefficient = jnp.exp(jax.random.uniform(keys[3], (HEADS, SEQ // BLOCK), jnp.float32, jnp.log(0.5), jnp.log(2.0)))
    fading_coefficient = jnp.repeat(fading_coefficient, BLOCK, axis=1)
    spots = jax.random.randint(keys[4], (3,), 0, SEQ)
    survival_ratio = jax.random.uniform(keys[5], (HEADS, 3), jnp.float32, 0.6, 0.8)
    paired_elements = (jnp.arange(SEQ)[None, :] == spots[:, None]).astype(jnp.float32)
    tile_bundles = jnp.dot(jnp.log(survival_ratio), paired_elements)
    return -fading_pace * fading_coefficient + tile_bundles


def draw_residual(key, part):
    keys = jax.random.split(jax.random.fold_in(key, 13), 3)
    row_scale = jnp.exp(jax.random.uniform(keys[1], (SEQ, 1), jnp.float32, jnp.log(0.3), jnp.log(3.0)))
    column = jnp.arange(D, dtype=jnp.float32)[None, :] / D
    column_scale = 0.5 * 4.0 ** column * jnp.exp(jax.random.uniform(keys[2], (1, D), jnp.float32, jnp.log(0.7), jnp.log(1.4)))
    base = jnp.clip(jax.random.normal(keys[0], (SEQ, D), jnp.float32), -6.0, 6.0)
    return (base * row_scale * column_scale).astype(jnp.bfloat16)


def draw_norm_gain(key, part):
    noise_key = jax.random.fold_in(key, 19)
    column = jnp.arange(D, dtype=jnp.float32) / D
    noise = jax.random.uniform(noise_key, (D,), jnp.float32, 0.82, 1.18)
    return 0.5 * 4.0 ** column * noise


def block_scale(key, dims, cuts, low, largest):
    level, own = 1.0, jax.random.fold_in(key, 6)
    for position, blocks in cuts:
        steps = jnp.exp(jax.random.uniform(jax.random.fold_in(own, position), (blocks,), jnp.float32, low / len(cuts), largest / len(cuts)))
        level = level * jnp.repeat(steps, dims[position] // blocks).reshape([-1 if axis == position else 1 for axis in range(len(dims))])
    return level


def scatter_about(key, dims, deviation, reach, shards=(), kind=jnp.bfloat16):
    level = block_scale(key, dims, shards, -0.22, 0.18) if shards else 1.0
    values = jax.random.normal(key, dims, jnp.float32) * deviation * level
    return jnp.minimum(jnp.maximum(values, -reach), reach).astype(kind)


def setup_inputs(seed: int = 0) -> dict:
    streams_of = jax.random.split(jax.random.key(seed), 15)
    return {
        "queries": scatter_about(streams_of[0], (SEQ, HEADS * HD), 1.0, 6.0, ((0, 8), (1, 4))),
        "key_input": scatter_about(streams_of[1], (SEQ, HEADS * HD), 1.0, 6.0, ((0, 8), (1, 4))),
        "value_input": scatter_about(streams_of[2], (SEQ, HEADS * HD), 1.0, 6.0, ((0, 8), (1, 4))),
        "gate_input": scatter_about(streams_of[3], (SEQ, HEADS * HD), 1.0, 6.0, ((0, 8), (1, 4))),
        "log_decay": draw_log_decay(jax.random.fold_in(streams_of[14], 71), 0),
        "residual": draw_residual(jax.random.fold_in(streams_of[14], 71), 0),
        "out_weight": scatter_about(streams_of[6], (HEADS * HD, D), (HEADS * HD // 4) ** -0.5, 0.375, ((0, 4),)),
        "norm_gain": draw_norm_gain(jax.random.fold_in(streams_of[14], 71), 0),
        "norm_bias": scatter_about(streams_of[8], (D,), 0.3, 1.8, (), jnp.float32),
        "gate_weight": scatter_about(streams_of[9], (D, FF), D ** -0.5, 0.125, ((0, 8), (1, 4))),
        "up_weight": scatter_about(streams_of[10], (D, FF), D ** -0.5, 0.125, ((0, 8), (1, 4))),
        "down_weight": scatter_about(streams_of[11], (FF, D), FF ** -0.5, 0.078125, ((0, 4), (1, 8))),
        "final_gain": jnp.clip(1.0 + 0.18 * jax.random.normal(streams_of[12], (D,), jnp.float32), 0.1, 1.9),
        "final_bias": scatter_about(streams_of[13], (D,), 0.3, 1.8, (), jnp.float32),
    }


ALPHA = 2.0 ** 0.25
EPS = 1e-05
ROPE_BASE = 10000.0

def rotate(values, positions):
    half = values.shape[-1] // 2
    freqs = ROPE_BASE ** (-2.0 * jnp.arange(half, dtype=jnp.float32) / values.shape[-1])
    angles = positions[:, None] * freqs[None, :]
    cosine = jnp.cos(angles)[:, None, :]
    sine = jnp.sin(angles)[:, None, :]
    first = values[..., :half]
    latter_operand = values[..., half:]
    return jnp.concatenate([first * cosine - latter_operand * sine, first * sine + latter_operand * cosine], axis=-1)

def head_norm(retained):
    center = retained - lax.optimization_barrier(jnp.mean(retained, axis=-1, keepdims=True))
    spread = lax.optimization_barrier(jnp.mean(center * center, axis=-1, keepdims=True))
    return center * lax.rsqrt(spread + EPS)

def row_norm(summed, gain, bias):
    center = summed - lax.optimization_barrier(jnp.mean(summed, axis=-1, keepdims=True))
    spread = lax.optimization_barrier(jnp.mean(center * center, axis=-1, keepdims=True))
    return center * lax.rsqrt(spread + EPS) * gain + bias

def rounded_sum(left, right, groups):
    width = left.shape[1] // groups
    total = jnp.zeros((left.shape[0], right.shape[1]), jnp.float32)
    for group in range(groups):
        part = jnp.dot(left[:, group * width:(group + 1) * width], right[group * width:(group + 1) * width], preferred_element_type=jnp.float32).astype(jnp.bfloat16)
        part = lax.optimization_barrier(part)
        total = total + part.astype(jnp.float32)
    return total.astype(jnp.bfloat16)

def retention(queries, key_input, value_input, log_decay):
    seq = queries.shape[0]
    positions = jnp.arange(seq, dtype=jnp.float32)
    shaped = (seq, HEADS, HD)
    turned_q = rotate(queries.astype(jnp.float32).reshape(shaped), positions).astype(jnp.bfloat16)
    turned_k = rotate(key_input.astype(jnp.float32).reshape(shaped), positions).astype(jnp.bfloat16)
    blocks = seq // BLOCK
    per_block = (blocks, BLOCK, HEADS, HD)
    query_blocks = turned_q.reshape(per_block)
    key_blocks = turned_k.reshape(per_block)
    value_blocks = value_input.reshape(per_block)
    block_decay_factors = log_decay.T.reshape(blocks, BLOCK, HEADS)
    lower = jnp.arange(BLOCK)[:, None] >= jnp.arange(BLOCK)[None, :]

    def advance(state, pieces):
        query_here, key_here, value_here, decay_here = pieces
        query_wide = query_here.astype(jnp.float32)
        key_wide = key_here.astype(jnp.float32)
        value_broadened = value_here.astype(jnp.float32)
        cumul = jnp.cumsum(decay_here, axis=0)
        gaps = cumul[:, None, :] - cumul[None, :, :]
        damping = jnp.where(lower[:, :, None], jnp.exp(jnp.minimum(gaps, 0.0)), 0.0)
        scores = jnp.einsum('ihd,jhd->ijh', query_wide, key_wide)
        weights = (scores * damping).astype(jnp.bfloat16)
        inner = jnp.einsum('ijh,jhe->ihe', weights.astype(jnp.float32), value_broadened)
        outer = jnp.einsum('ihd,hde->ihe', query_wide * jnp.exp(cumul)[:, :, None], state, precision=lax.Precision.HIGHEST)
        ending = cumul[-1]
        keyed = key_wide * jnp.exp(ending[None, :] - cumul)[:, :, None]
        fresh = jnp.einsum('jhd,jhe->hde', keyed, value_broadened, precision=lax.Precision.HIGHEST)
        state = jnp.exp(ending)[:, None, None] * state + fresh
        return (state, inner + outer)
    start = jnp.zeros((HEADS, HD, HD), jnp.float32)
    _, retained = lax.scan(advance, start, (query_blocks, key_blocks, value_blocks, block_decay_factors))
    return retained.reshape(shaped)

def reference(queries, key_input, value_input, gate_input, log_decay, residual, out_weight, norm_gain, norm_bias, gate_weight, up_weight, down_weight, final_gain, final_bias):
    retained = retention(queries, key_input, value_input, log_decay)
    normed = head_norm(retained).reshape(SEQ, HEADS * HD)
    mixed_heads = (jax.nn.silu(gate_input.astype(jnp.float32)) * normed).astype(jnp.bfloat16)

    def finish(pieces):
        head_rows, stream_rows = pieces
        mix = rounded_sum(head_rows, out_weight, N_TP)
        settled = row_norm(ALPHA * stream_rows.astype(jnp.float32) + mix.astype(jnp.float32), norm_gain, norm_bias).astype(jnp.bfloat16)
        gate_acts = jnp.dot(settled, gate_weight, preferred_element_type=jnp.float32)
        lifted = jnp.dot(settled, up_weight, preferred_element_type=jnp.float32)
        latent_width = (jax.nn.silu(gate_acts) * lifted).astype(jnp.bfloat16)
        ffn = rounded_sum(latent_width, down_weight, N_TP)
        return row_norm(ALPHA * settled.astype(jnp.float32) + ffn.astype(jnp.float32), final_gain, final_bias).astype(jnp.bfloat16)
    updated = lax.map(finish, (mixed_heads.reshape(N_SP, TOK_DEV, HEADS * HD), residual.reshape(N_SP, TOK_DEV, D)))
    return updated.reshape(SEQ, D)
```

```python
import functools

import jax
import jax.numpy as jnp
from jax import lax
from jax.experimental import pallas as pl
from jax.experimental.pallas import tpu as pltpu
from jax.sharding import PartitionSpec as P

MESH = pl.DeviceIdType.MESH

HD = 128
BLOCK = 128


ALPHA = 2.0**0.25
EPS = 1e-05
ROPE_BASE = 10000.0


def prefix(x, axis, combine, identity):
    peers, position = (lax.axis_size(axis), lax.axis_index(axis))
    everything = jax.tree.map(
        lambda part, kind: lax.all_gather(part.astype(kind), axis), x, (jnp.bfloat16, jnp.bfloat16)
    )
    start = jax.tree.map(
        lambda part, zero: jnp.broadcast_to(jnp.asarray(zero, part.dtype), part.shape), x, identity
    )

    def hop(k, before):
        reached = k < position
        new = combine(
            before, jax.tree.map(lambda part, own: part[k].astype(own.dtype), everything, x)
        )
        return jax.tree.map(lambda a, b: jnp.where(reached, a, b), new, before)

    return lax.fori_loop(0, peers, hop, start)


def rotate(values, positions):
    half = values.shape[-1] // 2
    freqs = ROPE_BASE ** (-2.0 * jnp.arange(half, dtype=jnp.float32) / values.shape[-1])
    angles = positions[:, None] * freqs[None, :]
    cosine = jnp.cos(angles)[:, None, :]
    sine = jnp.sin(angles)[:, None, :]
    first = values[..., :half]
    latter_operand = values[..., half:]
    return jnp.concatenate(
        [first * cosine - latter_operand * sine, first * sine + latter_operand * cosine], axis=-1
    )


def head_norm(retained):
    center = retained - jnp.mean(retained, axis=-1, keepdims=True)
    spread = jnp.mean(center * center, axis=-1, keepdims=True)
    return center * lax.rsqrt(spread + EPS)


def combine_states(earlier, later):
    return (earlier[0] * later[0], later[1] + later[0][:, None, None] * earlier[1])


def second_norm(second_sum, width, gain, bias):
    totals_two, squares_two = lax.psum(
        (jnp.sum(second_sum, axis=1), jnp.sum(second_sum * second_sum, axis=1)), "tp"
    )
    average_two = totals_two / width
    spread_two = squares_two / width - average_two * average_two
    scaled_two = (second_sum - average_two[:, None]) * lax.rsqrt(spread_two + EPS)[:, None]
    return (scaled_two * gain + bias).astype(jnp.bfloat16)


def layer_kernel(
    n_sp, n_tp,
    qs_ref, ret_ref, gin_ref, state_ref, res_ref, ow_ref, gain_ref, bias_ref, g_ref, u_ref, d_ref,
    out_ref,
    st, ow, gw, uw, dw, mixed, settled, hidden, keep, csend, crecv, fsend, frecv,
    st_s, st_r, ow_s, ow_r, wz_s, wy_s, w_r, mx_s, mx_r, se_s, se_r, c_s, c_r, f_s, f_r, lo,
):
    sp, tp = lax.axis_index("sp"), lax.axis_index("tp")
    rows = ret_ref.shape[0]
    outer_n = n_sp // 2
    o, i = sp // 2, lax.rem(sp, 2)
    x, c = tp // 2, lax.rem(tp, 2)
    half = lax.rem(o, 2)
    o_mate = o + 1 - 2 * half
    sp_mate = 2 * o_mate + i
    kr = g_ref.shape[1]

    def rem_copy(src, dst, ss, rs, dev):
        return pltpu.make_async_remote_copy(
            src_ref=src, dst_ref=dst, send_sem=ss, recv_sem=rs, device_id=dev, device_id_type=MESH
        )

    sp_peers = [(lax.rem(sp + j, n_sp), tp) for j in range(1, n_sp)]
    tp_peers = [(sp, lax.rem(tp + j, n_tp)) for j in range(1, n_tp)]
    diag = (sp_mate, 2 * (1 - x) + c)
    barrier = pltpu.get_barrier_semaphore()
    for dev in sp_peers + tp_peers + [diag]:
        pl.semaphore_signal(barrier, inc=1, device_id=dev, device_id_type=MESH)
    pl.semaphore_wait(barrier, n_sp + n_tp - 1)

    sends = []

    def go(copy):
        copy.start()
        sends.append(copy)

    local = [
        pltpu.make_async_copy(state_ref, st.at[sp], lo.at[0]),
        pltpu.make_async_copy(ow_ref, ow.at[tp], lo.at[1]),
    ]
    for j, dev in enumerate(sp_peers):
        go(rem_copy(state_ref, st.at[sp], st_s.at[j], st_r.at[sp], dev))
    for j, dev in enumerate(tp_peers):
        go(rem_copy(ow_ref, ow.at[tp], ow_s.at[j], ow_r.at[tp], dev))

    def slot(w, s):
        if w == 2:
            return dw.at[s]
        return (gw, uw)[w].at[pl.ds(pl.multiple_of(s * kr, kr), kr)]

    sources = (g_ref, u_ref, d_ref)
    y_mate = (2 * o + 1 - i, tp)
    for w in range(3):
        for j in range(1, outer_n):
            o_to = lax.rem(o + j, outer_n)
            go(rem_copy(sources[w].at[lax.rem(o_to, 2)], slot(w, sp), wz_s.at[w, j], w_r.at[w, sp], (2 * o_to + i, tp)))
        go(rem_copy(sources[w].at[half], slot(w, sp), wy_s.at[w, 0], w_r.at[w, sp], y_mate))
        local.append(pltpu.make_async_copy(sources[w].at[half], slot(w, sp), lo.at[2 + w]))
    for copy in local:
        copy.start()

    def arrived(w, s):
        rem_copy(slot(w, s), slot(w, s), wy_s.at[w, 0], w_r.at[w, s], y_mate).wait_recv()

    local[0].wait()
    for j in range(1, n_sp):
        s = lax.rem(sp + n_sp - j, n_sp)
        rem_copy(st.at[s], st.at[s], st_s.at[0], st_r.at[s], y_mate).wait_recv()
    heads = ret_ref.shape[1] // HD
    for h in range(heads):
        total = jnp.zeros((HD, HD), jnp.float32)
        for k in range(n_sp):
            decay = st[k, h, HD : HD + 1, :].astype(jnp.float32)
            total = jnp.where(k < sp, total * decay + st[k, h, :HD, :].astype(jnp.float32), total)
        entering = total.astype(jnp.bfloat16)
        cols = slice(h * HD, (h + 1) * HD)
        got = ret_ref[:, cols] + jnp.dot(qs_ref[:, cols], entering, preferred_element_type=jnp.float32)
        gate = gin_ref[:, cols].astype(jnp.float32)
        mixed[tp, :, cols] = (jax.nn.silu(gate) * head_norm(got)).astype(jnp.bfloat16)
    for j, dev in enumerate(tp_peers):
        go(rem_copy(mixed.at[tp], mixed.at[tp], mx_s.at[j], mx_r.at[tp], dev))
    local[1].wait()
    for j in range(1, n_tp):
        t = lax.rem(tp + j, n_tp)
        rem_copy(ow.at[t], ow.at[t], ow_s.at[0], ow_r.at[t], y_mate).wait_recv()
        rem_copy(mixed.at[t], mixed.at[t], mx_s.at[0], mx_r.at[t], y_mate).wait_recv()

    def settle(r, carry):
        here = pl.ds(pl.multiple_of(r * BLOCK, BLOCK), BLOCK)
        first = ALPHA * res_ref[here, :].astype(jnp.float32)
        for t in range(n_tp):
            first = first + jnp.dot(mixed[t, here, :], ow[t], preferred_element_type=jnp.float32)
        center = first - jnp.mean(first, axis=1, keepdims=True)
        spread = jnp.mean(center * center, axis=1, keepdims=True)
        settled[0, here, :] = (center * lax.rsqrt(spread + EPS) * gain_ref[...] + bias_ref[...]).astype(jnp.bfloat16)
        return carry

    lax.fori_loop(0, rows // BLOCK, settle, 0)
    mate = (sp_mate, tp)
    go(rem_copy(settled.at[0], settled.at[1], se_s.at[0], se_r.at[0], mate))

    for w in range(3):
        local[2 + w].wait()
        for j in range(1, outer_n):
            o_from = lax.rem(o + outer_n - j, outer_n)
            s = 2 * o_from + i
            arrived(w, s)
            go(rem_copy(slot(w, s), slot(w, s), wy_s.at[w, j], w_r.at[w, s], y_mate))
        if w == 1:
            for ww in range(2):
                for j in range(outer_n):
                    arrived(ww, 2 * lax.rem(o + outer_n - j, outer_n) + 1 - i)
            chunk = rows // 2

            def lift(r, carry, block):
                here = pl.ds(pl.multiple_of(r * chunk, chunk), chunk)
                lhs = settled[block, here, :]
                gate = jnp.dot(lhs, gw[...], preferred_element_type=jnp.float32)
                lifted = jnp.dot(lhs, uw[...], preferred_element_type=jnp.float32)
                hidden[block, here, :] = (jax.nn.silu(gate) * lifted).astype(jnp.bfloat16)
                return carry

            lax.fori_loop(0, 2, functools.partial(lift, block=0), 0)
    rem_copy(settled.at[0], settled.at[1], se_s.at[0], se_r.at[0], mate).wait_recv()
    lax.fori_loop(0, 2, functools.partial(lift, block=1), 0)
    for j in range(outer_n):
        arrived(2, 2 * lax.rem(o + outer_n - j, outer_n) + 1 - i)

    per_out = n_sp // n_tp
    kc = d_ref.shape[2]
    c_mate = (sp, 2 * x + 1 - c)
    targets = (diag, mate, (sp, 2 * (1 - x) + c))

    def finish(q):
        rem_copy(csend.at[q], crecv.at[q], c_s.at[q], c_r.at[q], c_mate).wait_recv()
        if q < 3:
            fsend[q] = (keep[q].astype(jnp.float32) + crecv[q].astype(jnp.float32)).astype(jnp.bfloat16)
            go(rem_copy(fsend.at[q], frecv.at[q], f_s.at[q], f_r.at[q], targets[q]))

    for q in range(4):
        block = 1 if q < 2 else 0
        xb = 1 - x if q in (0, 2) else x

        def project(r, carry, block=block, xb=xb, q=q):
            here = pl.ds(pl.multiple_of(r * chunk, chunk), chunk)
            lhs = hidden[block, here, :]
            for k in range(per_out):
                cols = slice(k * kc, (k + 1) * kc)
                other = dw[(2 * xb + 1 - c) * per_out + k]
                csend[q, here, cols] = jnp.dot(lhs, other, preferred_element_type=jnp.float32).astype(jnp.bfloat16)
                own = dw[(2 * xb + c) * per_out + k]
                keep[q, here, cols] = jnp.dot(lhs, own, preferred_element_type=jnp.float32).astype(jnp.bfloat16)
            return carry

        lax.fori_loop(0, 2, project, 0)
        go(rem_copy(csend.at[q], crecv.at[q], c_s.at[q], c_r.at[q], c_mate))
        if q > 0:
            finish(q - 1)
    finish(3)
    for q in range(3):
        rem_copy(fsend.at[q], frecv.at[q], f_s.at[q], f_r.at[q], targets[q]).wait_recv()
    width = out_ref.shape[1]
    mine = settled[0, :, pl.ds(pl.multiple_of(tp * width, width), width)].astype(jnp.float32)
    total = keep[3].astype(jnp.float32) + crecv[3].astype(jnp.float32)
    for q in range(3):
        total = total + frecv[q].astype(jnp.float32)
    out_ref[...] = ALPHA * mine + total
    for copy in sends:
        copy.wait_send()


def fused_layer(qs, retained, gate_in, state, residual, out_weight, gain, bias, gate_w, up_w, down_w, n_sp, n_tp):
    rows, width = residual.shape
    kr, ff = gate_w.shape
    hf = ff // 2
    hw = qs.shape[1]
    cols = width // n_tp
    halves = lambda w: jnp.transpose(w.reshape(kr, 2, hf), (1, 0, 2))
    down = down_w.reshape(2, hf, down_w.shape[1])
    bf = jnp.bfloat16
    vm, hb = pl.BlockSpec(memory_space=pltpu.VMEM), pl.BlockSpec(memory_space=pl.ANY)
    dma = lambda *shape: pltpu.SemaphoreType.DMA(shape)
    return pl.pallas_call(
        functools.partial(layer_kernel, n_sp, n_tp),
        out_shape=jax.ShapeDtypeStruct((rows, cols), jnp.float32),
        in_specs=[vm, vm, vm, hb, vm, hb, vm, vm, hb, hb, hb],
        out_specs=vm,
        scratch_shapes=[
            pltpu.VMEM((n_sp,) + state.shape, bf),
            pltpu.VMEM((n_tp,) + out_weight.shape, bf),
            pltpu.VMEM((n_sp * kr, hf), bf),
            pltpu.VMEM((n_sp * kr, hf), bf),
            pltpu.VMEM((n_sp, hf, down.shape[2]), bf),
            pltpu.VMEM((n_tp, rows, hw), bf),
            pltpu.VMEM((2, rows, width), bf),
            pltpu.VMEM((2, rows, hf), bf),
            pltpu.VMEM((4, rows, cols), bf),
            pltpu.VMEM((4, rows, cols), bf),
            pltpu.VMEM((4, rows, cols), bf),
            pltpu.VMEM((3, rows, cols), bf),
            pltpu.VMEM((3, rows, cols), bf),
            dma(n_sp), dma(n_sp), dma(n_tp), dma(n_tp),
            dma(3, n_sp // 2), dma(3, n_sp // 2), dma(3, n_sp),
            dma(n_tp), dma(n_tp), dma(1), dma(1), dma(4), dma(4), dma(3), dma(3), dma(5),
        ],
        compiler_params=pltpu.CompilerParams(collective_id=0, has_side_effects=True, vmem_limit_bytes=63 * 1024 * 1024),
    )(qs, retained, gate_in, state, residual, out_weight, gain[None], bias[None], halves(gate_w), halves(up_w), down)


def shards(
    queries,
    key_input,
    value_input,
    gate_input,
    log_decay,
    residual,
    out_weight,
    norm_gain,
    norm_bias,
    gate_weight,
    up_weight,
    down_weight,
    final_gain,
    final_bias,
):
    rows = queries.shape[0]
    heads_here = queries.shape[1] // HD
    blocks = rows // BLOCK
    offset = lax.axis_index("sp") * rows
    positions = (offset + jnp.arange(rows, dtype=jnp.int32)).astype(jnp.float32)
    shaped = (rows, heads_here, HD)
    per_block = (blocks, BLOCK, heads_here, HD)
    turned_q = (
        rotate(queries.astype(jnp.float32).reshape(shaped), positions)
        .astype(jnp.bfloat16)
        .reshape(per_block)
    )
    turned_k = (
        rotate(key_input.astype(jnp.float32).reshape(shaped), positions)
        .astype(jnp.bfloat16)
        .reshape(per_block)
    )
    value_blocks = value_input.reshape(per_block)
    cumul = jnp.cumsum(
        jnp.transpose(log_decay.reshape(heads_here, blocks, BLOCK), (1, 0, 2)), axis=2
    )
    cumul_rows = jnp.transpose(cumul, (0, 2, 1))
    lower = jnp.arange(BLOCK)[:, None] >= jnp.arange(BLOCK)[None, :]
    gaps = cumul[:, :, :, None] - cumul[:, :, None, :]
    damping = jnp.where(lower[None, None], jnp.exp(jnp.minimum(gaps, 0.0)), 0.0)
    scores = jnp.einsum("nihd,njhd->nhij", turned_q, turned_k, preferred_element_type=jnp.float32)
    weights = (scores * damping).astype(jnp.bfloat16)
    inner = jnp.einsum("nhij,njhe->nihe", weights, value_blocks, preferred_element_type=jnp.float32)
    ending = cumul[:, :, -1]
    value_broadened = value_blocks.astype(jnp.float32)
    keyed = turned_k.astype(jnp.float32) * jnp.exp(ending[:, None, :] - cumul_rows)[:, :, :, None]
    fresh = jnp.einsum("njhd,njhe->nhde", keyed, value_broadened, precision=lax.Precision.HIGHEST)

    def advance(state, pieces):
        decay_here, fresh_here = pieces
        return (jnp.exp(decay_here)[:, None, None] * state + fresh_here, state)

    local_state, prefixes = lax.scan(
        advance, jnp.zeros((heads_here, HD, HD), jnp.float32), (ending, fresh)
    )
    before = jnp.cumsum(ending, axis=0) - ending
    device_decay = jnp.exp(jnp.sum(ending, axis=0))
    n_sp, n_tp = lax.axis_size("sp"), lax.axis_size("tp")
    width = residual.shape[1]
    col_width = width // n_tp
    col_start = lax.axis_index("tp") * col_width

    def own_columns(array):
        return lax.dynamic_slice_in_dim(array, col_start, col_width, array.ndim - 1)

    if n_sp % 4 == 0 and n_tp == 4 and heads_here % 2 == 0 and gate_weight.shape[0] % 128 == 0:
        query_wide = turned_q.astype(jnp.float32) * jnp.exp(cumul_rows)[:, :, :, None]
        near = jnp.einsum("nihd,nhde->nihe", query_wide.astype(jnp.bfloat16), prefixes.astype(jnp.bfloat16), preferred_element_type=jnp.float32)
        far = (query_wide * jnp.exp(before)[:, None, :, None]).astype(jnp.bfloat16)
        tail = jnp.broadcast_to(device_decay[:, None, None], (heads_here, 16, HD))
        state = jnp.concatenate([local_state, tail], axis=1).astype(jnp.bfloat16)
        flat = (rows, heads_here * HD)
        second_sum = fused_layer(
            far.reshape(flat), (inner + near).reshape(flat), gate_input, state, residual, out_weight,
            norm_gain, norm_bias, gate_weight, up_weight, down_weight, n_sp, n_tp,
        )
        return second_norm(second_sum, width, own_columns(final_gain), own_columns(final_bias))
    scanned = prefix(
        (device_decay, local_state),
        "sp",
        combine_states,
        (jnp.ones_like(device_decay), jnp.zeros_like(local_state)),
    )
    entering = prefixes + jnp.exp(before)[:, :, None, None] * scanned[1][None]
    query_wide = turned_q.astype(jnp.float32) * jnp.exp(cumul_rows)[:, :, :, None]
    outer = jnp.einsum("nihd,nhde->nihe", query_wide, entering, precision=lax.Precision.HIGHEST)
    normed = head_norm((inner + outer).reshape(shaped)).reshape(rows, heads_here * HD)
    mixed_heads = (jax.nn.silu(gate_input.astype(jnp.float32)) * normed).astype(jnp.bfloat16)
    partial_value = jnp.dot(mixed_heads, out_weight, preferred_element_type=jnp.float32)
    mix = lax.psum(partial_value.astype(jnp.bfloat16), "tp")
    leading_sum = ALPHA * residual.astype(jnp.float32) + mix.astype(jnp.float32)
    center = leading_sum - jnp.mean(leading_sum, axis=1, keepdims=True)
    spread = jnp.mean(center * center, axis=1, keepdims=True)
    settled = (center * lax.rsqrt(spread + EPS) * norm_gain + norm_bias).astype(jnp.bfloat16)
    settled_cols = own_columns(settled)

    def add_rows(piece):
        return jnp.dot(settled, piece, preferred_element_type=jnp.float32)

    gate_acts = add_rows(lax.all_gather(gate_weight, "sp", axis=0, tiled=True))
    lifted = add_rows(lax.all_gather(up_weight, "sp", axis=0, tiled=True))
    latent_width = (jax.nn.silu(gate_acts) * lifted).astype(jnp.bfloat16)
    terms = jnp.dot(
        latent_width,
        lax.all_gather(down_weight, "sp", axis=1, tiled=True),
        preferred_element_type=jnp.float32,
    )
    ffn_cols = lax.psum_scatter(terms.astype(jnp.bfloat16), "tp", scatter_dimension=1, tiled=True)
    second_sum = ALPHA * settled_cols.astype(jnp.float32) + ffn_cols.astype(jnp.float32)
    return second_norm(second_sum, width, own_columns(final_gain), own_columns(final_bias))


def solution(mesh):
    in_specs = (
        P("sp", "tp"),
        P("sp", "tp"),
        P("sp", "tp"),
        P("sp", "tp"),
        P("tp", "sp"),
        P("sp", None),
        P("tp", None),
        P(),
        P(),
        P("sp", "tp"),
        P("sp", "tp"),
        P("tp", "sp"),
        P(),
        P(),
    )
    out_specs = P("sp", "tp")
    return jax.shard_map(shards, mesh=mesh, in_specs=in_specs, out_specs=out_specs, check_vma=False)
```

```python
import functools

import jax
import jax.numpy as jnp
from jax import lax
from jax.experimental import pallas as pl
from jax.experimental.pallas import tpu as pltpu
from jax.sharding import PartitionSpec as P

MESH = pl.DeviceIdType.MESH

HD = 128
BLOCK = 128


ALPHA = 2.0**0.25
EPS = 1e-05
ROPE_BASE = 10000.0


def prefix(x, axis, combine, identity):
    peers, position = (lax.axis_size(axis), lax.axis_index(axis))
    everything = jax.tree.map(
        lambda part, kind: lax.all_gather(part.astype(kind), axis), x, (jnp.bfloat16, jnp.bfloat16)
    )
    start = jax.tree.map(
        lambda part, zero: jnp.broadcast_to(jnp.asarray(zero, part.dtype), part.shape), x, identity
    )

    def hop(k, before):
        reached = k < position
        new = combine(
            before, jax.tree.map(lambda part, own: part[k].astype(own.dtype), everything, x)
        )
        return jax.tree.map(lambda a, b: jnp.where(reached, a, b), new, before)

    return lax.fori_loop(0, peers, hop, start)


def rotate(values, positions):
    half = values.shape[-1] // 2
    freqs = ROPE_BASE ** (-2.0 * jnp.arange(half, dtype=jnp.float32) / values.shape[-1])
    angles = positions[:, None] * freqs[None, :]
    cosine = jnp.cos(angles)[:, None, :]
    sine = jnp.sin(angles)[:, None, :]
    first = values[..., :half]
    latter_operand = values[..., half:]
    return jnp.concatenate(
        [first * cosine - latter_operand * sine, first * sine + latter_operand * cosine], axis=-1
    )


def head_norm(retained):
    center = retained - jnp.mean(retained, axis=-1, keepdims=True)
    spread = jnp.mean(center * center, axis=-1, keepdims=True)
    return center * lax.rsqrt(spread + EPS)


def combine_states(earlier, later):
    return (earlier[0] * later[0], later[1] + later[0][:, None, None] * earlier[1])


def second_norm(second_sum, width, gain, bias):
    totals_two, squares_two = lax.psum(
        (jnp.sum(second_sum, axis=1), jnp.sum(second_sum * second_sum, axis=1)), "tp"
    )
    average_two = totals_two / width
    spread_two = squares_two / width - average_two * average_two
    scaled_two = (second_sum - average_two[:, None]) * lax.rsqrt(spread_two + EPS)[:, None]
    return (scaled_two * gain + bias).astype(jnp.bfloat16)


def layer_kernel(
    n_sp, n_tp,
    qs_ref, ret_ref, gin_ref, state_ref, res_ref, ow_ref, gain_ref, bias_ref, g_ref, u_ref, d_ref,
    out_ref,
    st, ow, gw, uw, dw, mixed, settled, hidden, keep, csend, crecv, fsend, frecv,
    st_s, st_r, ow_s, ow_r, wz_s, wy_s, w_r, mx_s, mx_r, se_s, se_r, c_s, c_r, f_s, f_r, lo,
):
    sp, tp = lax.axis_index("sp"), lax.axis_index("tp")
    rows = ret_ref.shape[0]
    outer_n = n_sp // 2
    o, i = sp // 2, lax.rem(sp, 2)
    x, c = tp // 2, lax.rem(tp, 2)
    half = lax.rem(o, 2)
    o_mate = o + 1 - 2 * half
    sp_mate = 2 * o_mate + i
    kr = g_ref.shape[1]

    def rem_copy(src, dst, ss, rs, dev):
        return pltpu.make_async_remote_copy(
            src_ref=src, dst_ref=dst, send_sem=ss, recv_sem=rs, device_id=dev, device_id_type=MESH
        )

    sp_peers = [(lax.rem(sp + j, n_sp), tp) for j in range(1, n_sp)]
    tp_peers = [(sp, lax.rem(tp + j, n_tp)) for j in range(1, n_tp)]
    diag = (sp_mate, 2 * (1 - x) + c)
    barrier = pltpu.get_barrier_semaphore()
    for dev in sp_peers + tp_peers + [diag]:
        pl.semaphore_signal(barrier, inc=1, device_id=dev, device_id_type=MESH)
    pl.semaphore_wait(barrier, n_sp + n_tp - 1)

    sends = []

    def go(copy):
        copy.start()
        sends.append(copy)

    local = [
        pltpu.make_async_copy(state_ref, st.at[sp], lo.at[0]),
        pltpu.make_async_copy(ow_ref, ow.at[tp], lo.at[1]),
    ]
    for j, dev in enumerate(sp_peers):
        go(rem_copy(state_ref, st.at[sp], st_s.at[j], st_r.at[sp], dev))
    c_mate, x_mate = (sp, 2 * x + 1 - c), (sp, 2 * (1 - x) + c)
    from_c, from_x, from_d = 2 * x + 1 - c, 2 * (1 - x) + c, 2 * (1 - x) + 1 - c
    go(rem_copy(ow_ref, ow.at[tp], ow_s.at[0], ow_r.at[tp], c_mate))
    go(rem_copy(ow_ref, ow.at[tp], ow_s.at[1], ow_r.at[tp], x_mate))

    def slot(w, s):
        if w == 2:
            return dw.at[s]
        return (gw, uw)[w].at[pl.ds(pl.multiple_of(s * kr, kr), kr)]

    sources = (g_ref, u_ref, d_ref)
    y_mate = (2 * o + 1 - i, tp)

    def spread(w):
        for j in range(1, outer_n):
            o_to = lax.rem(o + j, outer_n)
            go(rem_copy(sources[w].at[lax.rem(o_to, 2)], slot(w, sp), wz_s.at[w, j], w_r.at[w, sp], (2 * o_to + i, tp)))

    spread(0)
    spread(1)
    for w in range(3):
        go(rem_copy(sources[w].at[half], slot(w, sp), wy_s.at[w, 0], w_r.at[w, sp], y_mate))
        local.append(pltpu.make_async_copy(sources[w].at[half], slot(w, sp), lo.at[2 + w]))
    for copy in local:
        copy.start()

    def arrived(w, s):
        rem_copy(slot(w, s), slot(w, s), wy_s.at[w, 0], w_r.at[w, s], y_mate).wait_recv()

    def hand_on(w, j):
        s = 2 * lax.rem(o + outer_n - j, outer_n) + i
        arrived(w, s)
        go(rem_copy(slot(w, s), slot(w, s), wy_s.at[w, j], w_r.at[w, s], y_mate))

    local[0].wait()
    for j in range(1, n_sp):
        s = lax.rem(sp + n_sp - j, n_sp)
        rem_copy(st.at[s], st.at[s], st_s.at[0], st_r.at[s], y_mate).wait_recv()
    heads = ret_ref.shape[1] // HD
    for h in range(heads):
        total = jnp.zeros((HD, HD), jnp.float32)
        for k in range(n_sp):
            decay = st[k, h, HD : HD + 1, :].astype(jnp.float32)
            total = jnp.where(k < sp, total * decay + st[k, h, :HD, :].astype(jnp.float32), total)
        entering = total.astype(jnp.bfloat16)
        cols = slice(h * HD, (h + 1) * HD)
        got = ret_ref[:, cols] + jnp.dot(qs_ref[:, cols], entering, preferred_element_type=jnp.float32)
        gate = gin_ref[:, cols].astype(jnp.float32)
        mixed[tp, :, cols] = (jax.nn.silu(gate) * head_norm(got)).astype(jnp.bfloat16)
    go(rem_copy(mixed.at[tp], mixed.at[tp], mx_s.at[0], mx_r.at[tp], c_mate))
    go(rem_copy(mixed.at[tp], mixed.at[tp], mx_s.at[1], mx_r.at[tp], x_mate))
    hand_on(0, 1)
    local[1].wait()
    rem_copy(mixed.at[from_x], mixed.at[from_x], mx_s.at[2], mx_r.at[from_x], x_mate).wait_recv()
    go(rem_copy(mixed.at[from_x], mixed.at[from_x], mx_s.at[2], mx_r.at[from_x], c_mate))
    rem_copy(ow.at[from_x], ow.at[from_x], ow_s.at[2], ow_r.at[from_x], x_mate).wait_recv()
    go(rem_copy(ow.at[from_x], ow.at[from_x], ow_s.at[2], ow_r.at[from_x], c_mate))
    for t in (from_c, from_d):
        rem_copy(ow.at[t], ow.at[t], ow_s.at[2], ow_r.at[t], c_mate).wait_recv()
        rem_copy(mixed.at[t], mixed.at[t], mx_s.at[2], mx_r.at[t], c_mate).wait_recv()

    def settle(r, carry):
        here = pl.ds(pl.multiple_of(r * BLOCK, BLOCK), BLOCK)
        first = ALPHA * res_ref[here, :].astype(jnp.float32)
        for t in range(n_tp):
            first = first + jnp.dot(mixed[t, here, :], ow[t], preferred_element_type=jnp.float32)
        center = first - jnp.mean(first, axis=1, keepdims=True)
        spread = jnp.mean(center * center, axis=1, keepdims=True)
        settled[0, here, :] = (center * lax.rsqrt(spread + EPS) * gain_ref[...] + bias_ref[...]).astype(jnp.bfloat16)
        return carry

    lax.fori_loop(0, rows // BLOCK, settle, 0)
    mate = (sp_mate, tp)
    chunk = rows // 2
    mate = (sp_mate, tp)

    def part(block, k):
        return settled.at[block, pl.ds(pl.multiple_of(k * chunk, chunk), chunk)]

    go(rem_copy(part(0, c), part(1, c), se_s.at[0], se_r.at[c], mate))
    spread(2)
    for w in range(2):
        for j in range(1 if w else 2, outer_n):
            hand_on(w, j)
    for w in range(2):
        local[2 + w].wait()
        for j in range(outer_n):
            arrived(w, 2 * lax.rem(o + outer_n - j, outer_n) + 1 - i)

    def lift(r, carry, block):
        here = pl.ds(pl.multiple_of(r * chunk, chunk), chunk)
        lhs = settled[block, here, :]
        gate = jnp.dot(lhs, gw[...], preferred_element_type=jnp.float32)
        lifted = jnp.dot(lhs, uw[...], preferred_element_type=jnp.float32)
        hidden[block, here, :] = (jax.nn.silu(gate) * lifted).astype(jnp.bfloat16)
        return carry

    rem_copy(part(0, c), part(1, c), se_s.at[0], se_r.at[c], mate).wait_recv()
    go(rem_copy(part(1, c), part(1, c), se_s.at[1], se_r.at[c], c_mate))
    lax.fori_loop(0, 2, functools.partial(lift, block=0), 0)
    hand_on(2, 1)
    rem_copy(part(1, 1 - c), part(1, 1 - c), se_s.at[1], se_r.at[1 - c], c_mate).wait_recv()
    lax.fori_loop(0, 2, functools.partial(lift, block=1), 0)
    for j in range(2, outer_n):
        hand_on(2, j)
    local[4].wait()
    for j in range(outer_n):
        arrived(2, 2 * lax.rem(o + outer_n - j, outer_n) + 1 - i)

    per_out = n_sp // n_tp
    kc = d_ref.shape[2]
    targets = (diag, mate, (sp, 2 * (1 - x) + c))

    def finish(q):
        rem_copy(csend.at[q], crecv.at[q], c_s.at[q], c_r.at[q], c_mate).wait_recv()
        if q < 3:
            fsend[q] = (keep[q].astype(jnp.float32) + crecv[q].astype(jnp.float32)).astype(jnp.bfloat16)
            go(rem_copy(fsend.at[q], frecv.at[q], f_s.at[q], f_r.at[q], targets[q]))

    for q in range(4):
        block = 1 if q < 2 else 0
        xb = 1 - x if q in (0, 2) else x

        def project(r, carry, block=block, xb=xb, q=q):
            here = pl.ds(pl.multiple_of(r * chunk, chunk), chunk)
            lhs = hidden[block, here, :]
            for k in range(per_out):
                cols = slice(k * kc, (k + 1) * kc)
                other = dw[(2 * xb + 1 - c) * per_out + k]
                csend[q, here, cols] = jnp.dot(lhs, other, preferred_element_type=jnp.float32).astype(jnp.bfloat16)
                own = dw[(2 * xb + c) * per_out + k]
                keep[q, here, cols] = jnp.dot(lhs, own, preferred_element_type=jnp.float32).astype(jnp.bfloat16)
            return carry

        lax.fori_loop(0, 2, project, 0)
        go(rem_copy(csend.at[q], crecv.at[q], c_s.at[q], c_r.at[q], c_mate))
        if q > 0:
            finish(q - 1)
    finish(3)
    for q in range(3):
        rem_copy(fsend.at[q], frecv.at[q], f_s.at[q], f_r.at[q], targets[q]).wait_recv()
    width = out_ref.shape[1]
    mine = settled[0, :, pl.ds(pl.multiple_of(tp * width, width), width)].astype(jnp.float32)
    total = keep[3].astype(jnp.float32) + crecv[3].astype(jnp.float32)
    for q in range(3):
        total = total + frecv[q].astype(jnp.float32)
    out_ref[...] = ALPHA * mine + total
    for copy in sends:
        copy.wait_send()


def fused_layer(qs, retained, gate_in, state, residual, out_weight, gain, bias, gate_w, up_w, down_w, n_sp, n_tp):
    rows, width = residual.shape
    kr, ff = gate_w.shape
    hf = ff // 2
    hw = qs.shape[1]
    cols = width // n_tp
    halves = lambda w: jnp.transpose(w.reshape(kr, 2, hf), (1, 0, 2))
    down = down_w.reshape(2, hf, down_w.shape[1])
    bf = jnp.bfloat16
    vm, hb = pl.BlockSpec(memory_space=pltpu.VMEM), pl.BlockSpec(memory_space=pl.ANY)
    dma = lambda *shape: pltpu.SemaphoreType.DMA(shape)
    return pl.pallas_call(
        functools.partial(layer_kernel, n_sp, n_tp),
        out_shape=jax.ShapeDtypeStruct((rows, cols), jnp.float32),
        in_specs=[vm, vm, vm, hb, vm, hb, vm, vm, hb, hb, hb],
        out_specs=vm,
        scratch_shapes=[
            pltpu.VMEM((n_sp,) + state.shape, bf),
            pltpu.VMEM((n_tp,) + out_weight.shape, bf),
            pltpu.VMEM((n_sp * kr, hf), bf),
            pltpu.VMEM((n_sp * kr, hf), bf),
            pltpu.VMEM((n_sp, hf, down.shape[2]), bf),
            pltpu.VMEM((n_tp, rows, hw), bf),
            pltpu.VMEM((2, rows, width), bf),
            pltpu.VMEM((2, rows, hf), bf),
            pltpu.VMEM((4, rows, cols), bf),
            pltpu.VMEM((4, rows, cols), bf),
            pltpu.VMEM((4, rows, cols), bf),
            pltpu.VMEM((3, rows, cols), bf),
            pltpu.VMEM((3, rows, cols), bf),
            dma(n_sp), dma(n_sp), dma(n_tp), dma(n_tp),
            dma(3, n_sp // 2), dma(3, n_sp // 2), dma(3, n_sp),
            dma(n_tp), dma(n_tp), dma(2), dma(2), dma(4), dma(4), dma(3), dma(3), dma(5),
        ],
        compiler_params=pltpu.CompilerParams(collective_id=0, has_side_effects=True, vmem_limit_bytes=63 * 1024 * 1024),
    )(qs, retained, gate_in, state, residual, out_weight, gain[None], bias[None], halves(gate_w), halves(up_w), down)


def shards(
    queries,
    key_input,
    value_input,
    gate_input,
    log_decay,
    residual,
    out_weight,
    norm_gain,
    norm_bias,
    gate_weight,
    up_weight,
    down_weight,
    final_gain,
    final_bias,
):
    rows = queries.shape[0]
    heads_here = queries.shape[1] // HD
    blocks = rows // BLOCK
    offset = lax.axis_index("sp") * rows
    positions = (offset + jnp.arange(rows, dtype=jnp.int32)).astype(jnp.float32)
    shaped = (rows, heads_here, HD)
    per_block = (blocks, BLOCK, heads_here, HD)
    turned_q = (
        rotate(queries.astype(jnp.float32).reshape(shaped), positions)
        .astype(jnp.bfloat16)
        .reshape(per_block)
    )
    turned_k = (
        rotate(key_input.astype(jnp.float32).reshape(shaped), positions)
        .astype(jnp.bfloat16)
        .reshape(per_block)
    )
    value_blocks = value_input.reshape(per_block)
    cumul = jnp.cumsum(
        jnp.transpose(log_decay.reshape(heads_here, blocks, BLOCK), (1, 0, 2)), axis=2
    )
    cumul_rows = jnp.transpose(cumul, (0, 2, 1))
    lower = jnp.arange(BLOCK)[:, None] >= jnp.arange(BLOCK)[None, :]
    gaps = cumul[:, :, :, None] - cumul[:, :, None, :]
    damping = jnp.where(lower[None, None], jnp.exp(jnp.minimum(gaps, 0.0)), 0.0)
    scores = jnp.einsum("nihd,njhd->nhij", turned_q, turned_k, preferred_element_type=jnp.float32)
    weights = (scores * damping).astype(jnp.bfloat16)
    inner = jnp.einsum("nhij,njhe->nihe", weights, value_blocks, preferred_element_type=jnp.float32)
    ending = cumul[:, :, -1]
    value_broadened = value_blocks.astype(jnp.float32)
    keyed = turned_k.astype(jnp.float32) * jnp.exp(ending[:, None, :] - cumul_rows)[:, :, :, None]
    fresh = jnp.einsum("njhd,njhe->nhde", keyed, value_broadened, precision=lax.Precision.HIGHEST)

    def advance(state, pieces):
        decay_here, fresh_here = pieces
        return (jnp.exp(decay_here)[:, None, None] * state + fresh_here, state)

    local_state, prefixes = lax.scan(
        advance, jnp.zeros((heads_here, HD, HD), jnp.float32), (ending, fresh)
    )
    before = jnp.cumsum(ending, axis=0) - ending
    device_decay = jnp.exp(jnp.sum(ending, axis=0))
    n_sp, n_tp = lax.axis_size("sp"), lax.axis_size("tp")
    width = residual.shape[1]
    col_width = width // n_tp
    col_start = lax.axis_index("tp") * col_width

    def own_columns(array):
        return lax.dynamic_slice_in_dim(array, col_start, col_width, array.ndim - 1)

    if n_sp % 4 == 0 and n_tp == 4 and heads_here % 2 == 0 and gate_weight.shape[0] % 128 == 0:
        query_wide = turned_q.astype(jnp.float32) * jnp.exp(cumul_rows)[:, :, :, None]
        near = jnp.einsum("nihd,nhde->nihe", query_wide.astype(jnp.bfloat16), prefixes.astype(jnp.bfloat16), preferred_element_type=jnp.float32)
        far = (query_wide * jnp.exp(before)[:, None, :, None]).astype(jnp.bfloat16)
        tail = jnp.broadcast_to(device_decay[:, None, None], (heads_here, 16, HD))
        state = jnp.concatenate([local_state, tail], axis=1).astype(jnp.bfloat16)
        flat = (rows, heads_here * HD)
        second_sum = fused_layer(
            far.reshape(flat), (inner + near).reshape(flat), gate_input, state, residual, out_weight,
            norm_gain, norm_bias, gate_weight, up_weight, down_weight, n_sp, n_tp,
        )
        return second_norm(second_sum, width, own_columns(final_gain), own_columns(final_bias))
    scanned = prefix(
        (device_decay, local_state),
        "sp",
        combine_states,
        (jnp.ones_like(device_decay), jnp.zeros_like(local_state)),
    )
    entering = prefixes + jnp.exp(before)[:, :, None, None] * scanned[1][None]
    query_wide = turned_q.astype(jnp.float32) * jnp.exp(cumul_rows)[:, :, :, None]
    outer = jnp.einsum("nihd,nhde->nihe", query_wide, entering, precision=lax.Precision.HIGHEST)
    normed = head_norm((inner + outer).reshape(shaped)).reshape(rows, heads_here * HD)
    mixed_heads = (jax.nn.silu(gate_input.astype(jnp.float32)) * normed).astype(jnp.bfloat16)
    partial_value = jnp.dot(mixed_heads, out_weight, preferred_element_type=jnp.float32)
    mix = lax.psum(partial_value.astype(jnp.bfloat16), "tp")
    leading_sum = ALPHA * residual.astype(jnp.float32) + mix.astype(jnp.float32)
    center = leading_sum - jnp.mean(leading_sum, axis=1, keepdims=True)
    spread = jnp.mean(center * center, axis=1, keepdims=True)
    settled = (center * lax.rsqrt(spread + EPS) * norm_gain + norm_bias).astype(jnp.bfloat16)
    settled_cols = own_columns(settled)

    def add_rows(piece):
        return jnp.dot(settled, piece, preferred_element_type=jnp.float32)

    gate_acts = add_rows(lax.all_gather(gate_weight, "sp", axis=0, tiled=True))
    lifted = add_rows(lax.all_gather(up_weight, "sp", axis=0, tiled=True))
    latent_width = (jax.nn.silu(gate_acts) * lifted).astype(jnp.bfloat16)
    terms = jnp.dot(
        latent_width,
        lax.all_gather(down_weight, "sp", axis=1, tiled=True),
        preferred_element_type=jnp.float32,
    )
    ffn_cols = lax.psum_scatter(terms.astype(jnp.bfloat16), "tp", scatter_dimension=1, tiled=True)
    second_sum = ALPHA * settled_cols.astype(jnp.float32) + ffn_cols.astype(jnp.float32)
    return second_norm(second_sum, width, own_columns(final_gain), own_columns(final_bias))


def solution(mesh):
    in_specs = (
        P("sp", "tp"),
        P("sp", "tp"),
        P("sp", "tp"),
        P("sp", "tp"),
        P("tp", "sp"),
        P("sp", None),
        P("tp", None),
        P(),
        P(),
        P("sp", "tp"),
        P("sp", "tp"),
        P("tp", "sp"),
        P(),
        P(),
    )
    out_specs = P("sp", "tp")
    return jax.shard_map(shards, mesh=mesh, in_specs=in_specs, out_specs=out_specs, check_vma=False)
```
